1024 devices in a mesh: fs: 16 (over z), rep: 8 (over y), tp: 8 (over x, core).
Axes of the slice: x: 4, y: 8, z: 16, core: 2. Of those that a mesh axis runs over, the one named last changes fastest.
Arguments:
- saved_hidden: bfloat16 [114688, 2048], P(('fs', 'rep')), may hold values from -12 to 12
- grad_value: bfloat16 [114688, 1024], P(('fs', 'rep'), 'tp'), may hold values from -12 to 12
- saved_mixed: bfloat16 [114688, 1024], P(('fs', 'rep'), 'tp'), may hold values from -12 to 12
- grad_output: bfloat16 [114688, 2048], P(('fs', 'rep')), may hold values from -12 to 12
- basis_value: bfloat16 [2048, 128], replicated, may hold values from -0.5 to 0.5
- basis_output: bfloat16 [2048, 128], replicated, may hold values from -0.5 to 0.5
- weight_value: float32 [2048, 1024], P('fs', 'tp'), may hold values from -0.125 to 0.125
- weight_output: float32 [1024, 2048], P('tp', 'fs'), may hold values from -0.1875 to 0.1875
- first_value: float32 [128, 1024], P('fs', 'tp'), may hold values from -4 to 4
- second_value: float32 [128, 1024], P('fs', 'tp'), may hold values from 0.05 to 0.5
- first_output: float32 [128, 1024], P('fs', 'tp'), may hold values from -4 to 4
- second_output: float32 [128, 1024], P('fs', 'tp'), may hold values from 0.05 to 0.5
Outputs:
- step_value: float32 [2048, 1024], P('fs', 'tp')
- step_output: float32 [1024, 2048], P('tp', 'fs')
- new_weight_value: float32 [2048, 1024], P('fs', 'tp')
- new_weight_output: float32 [1024, 2048], P('tp', 'fs')
- copy_value: bfloat16 [2048, 1024], P(None, 'tp')
- copy_output: bfloat16 [1024, 2048], P('tp')
- new_first_value: float32 [128, 1024], P('fs', 'tp')
- new_second_value: float32 [128, 1024], P('fs', 'tp')
- new_first_output: float32 [128, 1024], P('fs', 'tp')
- new_second_output: float32 [128, 1024], P('fs', 'tp')
The draws below stay inside these ranges and needn't reach their ends.
All inputs are finite; a program needn't handle non-finite values.
Results may differ from the reference program's by a relative error of at most 0.0045.
Values may be sent and summed in bfloat16 or wider, within the bound.
No kernel may reach another device: no remote copies, remote signals or barrier semaphores. Data moves between devices by JAX's collectives and lax.ppermute only.
A program may use at most 32 MiB of HBM per device.

```python
import math
import jax
import jax.numpy as jnp
from jax import lax

D = 2048
AW = 1024
RANK = 128
TOKENS = 114688


def field_values(key, row_total, col_total, rising_columns):
    key_noise = jax.random.fold_in(key, 0)
    length = col_total if rising_columns else row_total
    position = jnp.arange(length, dtype=jnp.float32) / max(length - 1, 1)
    noise_field = jnp.clip(jax.random.normal(key_noise, (row_total, col_total), jnp.float32), -4.0, 4.0)
    scales = jnp.exp(math.log(3.0) * position)
    if rising_columns:
        return noise_field * scales[None, :]
    return noise_field * scales[:, None]


def draw_saved_hidden(key, part):
    return field_values(jax.random.fold_in(key, 11), TOKENS, D, False).astype(jnp.bfloat16)


def draw_grad_value(key, part):
    return field_values(jax.random.fold_in(key, 23), TOKENS, AW, True).astype(jnp.bfloat16)


def draw_saved_mixed(key, part):
    return field_values(jax.random.fold_in(key, 37), TOKENS, AW, True).astype(jnp.bfloat16)


def draw_grad_output(key, part):
    return field_values(jax.random.fold_in(key, 41), TOKENS, D, False).astype(jnp.bfloat16)


def steps_of(own_key, extent, cuts, smallest, top_value):
    loudness = 1.0
    for axis_at, shards_of in cuts:
        heights = jax.random.uniform(jax.random.fold_in(jax.random.fold_in(own_key, 6), axis_at), (shards_of,), jnp.float32, smallest / len(cuts), top_value / len(cuts))
        loudness = loudness * jnp.repeat(jnp.exp(heights), extent[axis_at] // shards_of).reshape((-1,) + (1,) * (len(extent) - 1 - axis_at))
    return loudness


def centred(rng, dims, scale, most, cuts=(), held_as=jnp.bfloat16):
    result = scale * jax.random.normal(rng, dims, jnp.float32)
    if cuts:
        result = result * steps_of(rng, dims, cuts, -0.22, 0.18)
    return jnp.clip(result, -most, most).astype(held_as)


def setup_inputs(seed: int = 0) -> dict:
    streams_of = jax.random.split(jax.random.key(seed), 13)
    return {
        "saved_hidden": draw_saved_hidden(jax.random.fold_in(streams_of[12], 71), 0),
        "grad_value": draw_grad_value(jax.random.fold_in(streams_of[12], 71), 0),
        "saved_mixed": draw_saved_mixed(jax.random.fold_in(streams_of[12], 71), 0),
        "grad_output": draw_grad_output(jax.random.fold_in(streams_of[12], 71), 0),
        "basis_value": centred(streams_of[4], (D, RANK), RANK ** -0.5, 0.5),
        "basis_output": centred(streams_of[5], (D, RANK), RANK ** -0.5, 0.5),
        "weight_value": centred(streams_of[6], (D, AW), D ** -0.5, 0.125, ((0, 16), (1, 8)), jnp.float32),
        "weight_output": centred(streams_of[7], (AW, D), AW ** -0.5, 0.1875, ((0, 8), (1, 16)), jnp.float32),
        "first_value": centred(streams_of[8], (RANK, AW), 1.0, 4.0, ((0, 16), (1, 8)), jnp.float32),
        "second_value": jnp.clip(jnp.exp(math.log(0.5) - 2.3025851 * jax.random.uniform(streams_of[9], (RANK, AW), jnp.float32) ** steps_of(streams_of[9], (RANK, AW), ((0, 16), (1, 8)), -0.2, 0.2)), 0.05, 0.5),
        "first_output": centred(streams_of[10], (RANK, AW), 1.0, 4.0, ((0, 16), (1, 8)), jnp.float32),
        "second_output": jnp.clip(jnp.exp(math.log(0.5) - 2.3025851 * jax.random.uniform(streams_of[11], (RANK, AW), jnp.float32) ** steps_of(streams_of[11], (RANK, AW), ((0, 16), (1, 8)), -0.2, 0.2)), 0.05, 0.5),
    }


first_decay = 0.8
second_decay = 0.9
learning_rate = 0.02
norm_epsilon = 1e-06

def project(basis, gradient):
    return jnp.dot(basis.astype(jnp.float32).T, gradient, precision=lax.Precision.HIGHEST)

def moments(projected, first_old, second_old, clip_factor):
    scaled = clip_factor * projected
    first_new = first_decay * first_old + (1.0 - first_decay) * scaled
    second_new = second_decay * second_old + (1.0 - second_decay) * scaled * scaled
    return (first_new, second_new, first_new / jnp.sqrt(second_new))

def reference(saved_hidden, grad_value, saved_mixed, grad_output, basis_value, basis_output, weight_value, weight_output, first_value, second_value, first_output, second_output):
    gradient_value = jnp.dot(saved_hidden.T, grad_value, preferred_element_type=jnp.float32)
    gradient_output = jnp.dot(grad_output.T, saved_mixed, preferred_element_type=jnp.float32)
    projected_value = project(basis_value, gradient_value)
    projected_output = project(basis_output, gradient_output)
    squares = jnp.sum(projected_value * projected_value) + jnp.sum(projected_output * projected_output)
    mean_square = squares / (2 * RANK * AW)
    clip_factor = jnp.minimum(1.0, 1.0 / jnp.sqrt(mean_square + norm_epsilon))
    first_new_value, second_new_value, direction_value = moments(projected_value, first_value, second_value, clip_factor)
    first_new_output, second_new_output, direction_output = moments(projected_output, first_output, second_output, clip_factor)
    step_value = jnp.dot(basis_value.astype(jnp.float32), direction_value, precision=lax.Precision.HIGHEST)
    step_output = jnp.dot(basis_output.astype(jnp.float32), direction_output, precision=lax.Precision.HIGHEST).T
    new_weight_value = weight_value - learning_rate * step_value
    new_weight_output = weight_output - learning_rate * step_output
    return (step_value, step_output, new_weight_value, new_weight_output, new_weight_value.astype(jnp.bfloat16), new_weight_output.astype(jnp.bfloat16), first_new_value, second_new_value, first_new_output, second_new_output)
```

```python
import jax
import jax.numpy as jnp
from jax import lax
from jax.sharding import PartitionSpec as P


AW = 1024
RANK = 128


first_decay = 0.8
second_decay = 0.9
learning_rate = 0.02
norm_epsilon = 1e-06
f32 = jnp.float32
bf16 = jnp.bfloat16
contract_leading = (((0,), (0,)), ((), ()))


def exchange(chunks, axes):
    return lax.all_to_all(chunks, axes, 0, 0, tiled=True)


def split(array):
    upper = array.astype(bf16)
    return upper, (array - upper.astype(f32)).astype(bf16)


def moments(projected, first_old, second_old, clip_factor):
    scaled = clip_factor * projected
    first_new = first_decay * first_old + (1.0 - first_decay) * scaled
    second_new = second_decay * second_old + (1.0 - second_decay) * scaled * scaled
    return (first_new, second_new, first_new / jnp.sqrt(second_new))


def split_product(reduced, other):
    upper, lower = split(reduced)
    stacked = jnp.concatenate([upper, lower], axis=1)
    both = lax.dot_general(stacked, other, contract_leading, preferred_element_type=f32)
    rank_count = reduced.shape[1]
    return both[:rank_count] + both[rank_count:]


def local(
    saved_hidden,
    grad_value,
    saved_mixed,
    grad_output,
    basis_value,
    basis_output,
    weight_value,
    weight_output,
    first_value,
    second_value,
    first_output,
    second_output,
):
    fs, rep, tp = lax.axis_size("fs"), lax.axis_size("rep"), lax.axis_size("tp")
    fs_index = lax.axis_index("fs")
    rep_index = lax.axis_index("rep")
    rows, columns = weight_value.shape
    cut = rows // rep
    ranks = first_value.shape[0]
    width = RANK // (rep * tp)

    old = jnp.stack([first_value, second_value, first_output, second_output])
    old_piece = lax.dynamic_slice_in_dim(old, rep_index, 1, 1).reshape(4, columns)
    old_upper, old_lower = split(old_piece)
    piece = jnp.concatenate(
        [
            lax.dynamic_slice_in_dim(weight_value, rep_index * cut, cut, 0).astype(bf16),
            lax.dynamic_slice_in_dim(weight_output, rep_index * cut, cut, 0).astype(bf16),
            old_upper,
            old_lower,
        ]
    )
    spread = jnp.broadcast_to(piece[None], (fs, *piece.shape))
    pieces = exchange(spread, "fs")
    gathered = lax.all_gather(pieces, "rep")

    reduced_hidden = jnp.dot(saved_hidden, basis_value, preferred_element_type=f32)
    reduced_output = jnp.dot(grad_output, basis_output, preferred_element_type=f32)
    part_value = split_product(reduced_hidden, grad_value)
    part_output = split_product(reduced_output, saved_mixed)

    part = jnp.stack(
        [part_value.reshape(-1, width, columns), part_output.reshape(-1, width, columns)], axis=1
    ).reshape(rep * tp, 2 * width, columns)
    part = exchange(part, ("rep", "tp"))
    part = jnp.sum(part.reshape(rep, tp, 2 * width, columns), axis=0)
    part = jnp.broadcast_to(part.astype(bf16)[None], (fs, *part.shape))
    part = exchange(part.reshape(fs, tp * 2 * width, columns), "fs")
    whole = jnp.sum(part.astype(f32), axis=0).reshape(tp, 2 * width, columns)

    squares = jnp.broadcast_to(jnp.sum(whole * whole), (tp, 1, columns))
    square_upper, square_lower = split(squares)
    back = jnp.concatenate(
        [whole.astype(bf16), square_upper, square_lower, square_lower, square_lower], axis=1
    )[:, :8]
    back = jnp.broadcast_to(back[None], (rep, *back.shape)).reshape(rep * tp, *back.shape[1:])
    back = exchange(back, ("rep", "tp")).astype(f32)
    projected_value = back[:, :width].reshape(RANK, columns)
    projected_output = back[:, width : 2 * width].reshape(RANK, columns)
    total_squares = jnp.sum(back[:, 2 * width, 0] + back[:, 2 * width + 1, 0])
    mean_square = total_squares / (2 * RANK * AW)
    clip_factor = jnp.minimum(1.0, 1.0 / jnp.sqrt(mean_square + norm_epsilon))

    old = gathered[:, :, 2 * cut :].astype(f32)
    old = old[:, :, :4] + old[:, :, 4:]
    old = old.transpose(2, 1, 0, 3).reshape(4, RANK, columns)
    direction_value = moments(projected_value, old[0], old[1], clip_factor)[2]
    direction_output = moments(projected_output, old[2], old[3], clip_factor)[2]
    moment_first = fs_index * ranks
    new_first_value, new_second_value, _ = moments(
        lax.dynamic_slice_in_dim(projected_value, moment_first, ranks, 0),
        first_value,
        second_value,
        clip_factor,
    )
    new_first_output, new_second_output, _ = moments(
        lax.dynamic_slice_in_dim(projected_output, moment_first, ranks, 0),
        first_output,
        second_output,
        clip_factor,
    )

    value_upper, value_lower = split(direction_value)
    output_upper, output_lower = split(direction_output)

    def value_step(basis):
        return jnp.dot(basis, value_upper, preferred_element_type=f32) + jnp.dot(
            basis, value_lower, preferred_element_type=f32
        )

    def output_step(basis):
        across = (((0,), (1,)), ((), ()))
        return lax.dot_general(
            output_upper, basis, across, preferred_element_type=f32
        ) + lax.dot_general(output_lower, basis, across, preferred_element_type=f32)

    value_rows = lax.dynamic_slice_in_dim(basis_value, fs_index * rows, rows, 0)
    output_rows = lax.dynamic_slice_in_dim(basis_output, fs_index * rows, rows, 0)
    step_value = value_step(value_rows)
    step_output = output_step(output_rows)
    new_weight_value = weight_value - learning_rate * step_value
    new_weight_output = weight_output - learning_rate * step_output
    whole_value = gathered[:, :, :cut].transpose(1, 0, 2, 3).reshape(fs * rows, columns)
    whole_output = gathered[:, :, cut : 2 * cut].transpose(0, 2, 1, 3).reshape(rows, fs * columns)
    copy_value = (whole_value.astype(f32) - learning_rate * value_step(basis_value)).astype(bf16)
    copy_output = (whole_output.astype(f32) - learning_rate * output_step(basis_output)).astype(
        bf16
    )
    return (
        step_value,
        step_output,
        new_weight_value,
        new_weight_output,
        copy_value,
        copy_output,
        new_first_value,
        new_second_value,
        new_first_output,
        new_second_output,
    )


def solution(mesh):
    return jax.shard_map(
        local,
        mesh=mesh,
        in_specs=(
            P(("fs", "rep"), None),
            P(("fs", "rep"), "tp"),
            P(("fs", "rep"), "tp"),
            P(("fs", "rep"), None),
            P(),
            P(),
            P("fs", "tp"),
            P("tp", "fs"),
            P("fs", "tp"),
            P("fs", "tp"),
            P("fs", "tp"),
            P("fs", "tp"),
        ),
        out_specs=(
            P("fs", "tp"),
            P("tp", "fs"),
            P("fs", "tp"),
            P("tp", "fs"),
            P(None, "tp"),
            P("tp", None),
            P("fs", "tp"),
            P("fs", "tp"),
            P("fs", "tp"),
            P("fs", "tp"),
        ),
        check_vma=False,
    )
```

```python
import jax
import jax.numpy as jnp
from jax import lax
from jax.experimental import pallas as pl
from jax.experimental.pallas import tpu as pltpu
from jax.sharding import PartitionSpec as P


AW = 1024
RANK = 128


first_decay = 0.8
second_decay = 0.9
learning_rate = 0.02
norm_epsilon = 1e-06
f32 = jnp.float32
bf16 = jnp.bfloat16
contract_leading = (((0,), (0,)), ((), ()))
contract_trailing = (((1,), (1,)), ((), ()))


def exchange(chunks, axes):
    return lax.all_to_all(chunks, axes, 0, 0, tiled=True)


def split(array):
    upper = array.astype(bf16)
    return upper, (array - upper.astype(f32)).astype(bf16)


def moments(projected, first_old, second_old, clip_factor):
    scaled = clip_factor * projected
    first_new = first_decay * first_old + (1.0 - first_decay) * scaled
    second_new = second_decay * second_old + (1.0 - second_decay) * scaled * scaled
    return (first_new, second_new, first_new / jnp.sqrt(second_new))


def finish_kernel(
    fs_ref,
    rows_ref,
    wholes_ref,
    basis_value_ref,
    basis_output_ref,
    weight_value_ref,
    weight_output_ref,
    step_value_ref,
    step_output_ref,
    new_weight_value_ref,
    new_weight_output_ref,
    copy_value_ref,
    copy_output_ref,
    new_first_value_ref,
    new_second_value_ref,
    new_first_output_ref,
    new_second_output_ref,
    value_ref,
    output_ref,
):
    fs, _, columns = rows_ref.shape
    ranks = new_first_value_ref.shape[0]
    block = weight_value_ref.shape[0]
    cut = wholes_ref.shape[2] // 2
    total = rows_ref[0, 6 * ranks : 6 * ranks + 8, :]
    for i in range(1, fs):
        total = total + rows_ref[i, 6 * ranks : 6 * ranks + 8, :]
    mean_square = jnp.max(total, keepdims=True) / (2 * RANK * AW)
    clip_factor = jnp.minimum(1.0, 1.0 / jnp.sqrt(mean_square + norm_epsilon))

    def part(i, k):
        return rows_ref[i, k * ranks : (k + 1) * ranks, :]

    for i in range(fs):
        here = slice(i * ranks, (i + 1) * ranks)
        value_ref[here, :] = moments(part(i, 0), part(i, 2), part(i, 3), clip_factor)[2]
        output_ref[here, :] = moments(part(i, 1), part(i, 4), part(i, 5), clip_factor)[2]
    own = fs_ref[0]
    first, second, _ = moments(part(own, 0), part(own, 2), part(own, 3), clip_factor)
    new_first_value_ref[...] = first
    new_second_value_ref[...] = second
    first, second, _ = moments(part(own, 1), part(own, 4), part(own, 5), clip_factor)
    new_first_output_ref[...] = first
    new_second_output_ref[...] = second

    value_upper, value_lower = split(value_ref[...])
    output_upper, output_lower = split(output_ref[...].T)

    def value_step(basis):
        return jnp.dot(basis, value_upper, preferred_element_type=f32) + jnp.dot(
            basis, value_lower, preferred_element_type=f32
        )

    def output_step(basis):
        return lax.dot_general(
            output_upper, basis, contract_trailing, preferred_element_type=f32
        ) + lax.dot_general(output_lower, basis, contract_trailing, preferred_element_type=f32)

    own_rows = pl.ds(pl.multiple_of(own * block, block), block)
    step = value_step(basis_value_ref[own_rows, :])
    step_value_ref[...] = step
    new_weight_value_ref[...] = weight_value_ref[...] - learning_rate * step
    step = output_step(basis_output_ref[own_rows, :])
    step_output_ref[...] = step
    new_weight_output_ref[...] = weight_output_ref[...] - learning_rate * step
    for i in range(fs):
        here = slice(i * block, (i + 1) * block)
        whole = wholes_ref[:, i, :cut, :].reshape(block, columns).astype(f32)
        step = value_step(basis_value_ref[here, :])
        copy_value_ref[here, :] = (whole - learning_rate * step).astype(bf16)
        whole = wholes_ref[:, i, cut:, :].reshape(block, columns).astype(f32)
        step = output_step(basis_output_ref[here, :])
        copy_output_ref[:, here] = (whole - learning_rate * step).astype(bf16)


vmem = pl.BlockSpec(memory_space=pltpu.VMEM)
smem = pl.BlockSpec(memory_space=pltpu.SMEM)


def call(kernel, inputs, shapes, specs=None, scratch=(), flops=0, room=8, grid=None):
    outs = tuple(jax.ShapeDtypeStruct(s, t) for s, t in shapes)
    more = {} if grid is None else {"grid": grid}
    return pl.pallas_call(
        kernel,
        out_shape=outs,
        in_specs=[vmem] * len(inputs) if specs is None else specs,
        out_specs=tuple(vmem for _ in outs),
        scratch_shapes=scratch,
        compiler_params=pltpu.CompilerParams(vmem_limit_bytes=room * 2**20),
        cost_estimate=pl.CostEstimate(flops=flops, bytes_accessed=2**20, transcendentals=0),
        **more,
    )(*inputs)


def partial_kernel(
    rep_ref,
    hidden_ref,
    grad_value_ref,
    grad_output_ref,
    mixed_ref,
    basis_value_ref,
    basis_output_ref,
    weight_value_ref,
    weight_output_ref,
    out_ref,
    value_ref,
    output_ref,
):
    step = pl.program_id(0)

    @pl.when(step == 0)
    def _():
        value_ref[...] = jnp.zeros_like(value_ref)
        output_ref[...] = jnp.zeros_like(output_ref)

    for tokens_ref, basis_ref, other_ref, sum_ref in (
        (hidden_ref, basis_value_ref, grad_value_ref, value_ref),
        (grad_output_ref, basis_output_ref, mixed_ref, output_ref),
    ):
        reduced = jnp.dot(tokens_ref[...], basis_ref[...], preferred_element_type=f32)
        upper, lower = split(reduced)
        other = other_ref[...]
        sum_ref[...] += lax.dot_general(
            upper, other, contract_leading, preferred_element_type=f32
        ) + lax.dot_general(lower, other, contract_leading, preferred_element_type=f32)

    @pl.when(step == pl.num_programs(0) - 1)
    def _():
        fs, height, _ = out_ref.shape
        ranks = RANK // fs
        count = 2 * ranks
        cut = (height - 2 * count) // 2
        piece = pl.ds(pl.multiple_of(rep_ref[0] * cut, cut), cut)
        piece_value = weight_value_ref[piece, :].astype(bf16)
        piece_output = weight_output_ref[piece, :].astype(bf16)
        for i in range(fs):
            here = slice(i * ranks, (i + 1) * ranks)
            upper, lower = split(jnp.concatenate([value_ref[here, :], output_ref[here, :]]))
            out_ref[i, :count, :] = upper
            out_ref[i, count : 2 * count, :] = lower
            out_ref[i, 2 * count : 2 * count + cut, :] = piece_value
            out_ref[i, 2 * count + cut :, :] = piece_output


def partial(rep_index, hidden, grad_value, grad_output, mixed, bases, weights, fs, rep):
    tokens, depth = hidden.shape
    rows, columns = weights[0].shape
    steps = 4
    block = tokens // steps
    wide = pl.BlockSpec((block, depth), lambda i: (i, 0))
    narrow = pl.BlockSpec((block, columns), lambda i: (i, 0))
    height = 4 * (RANK // fs) + 2 * (rows // rep)
    return call(
        partial_kernel,
        (rep_index, hidden, grad_value, grad_output, mixed, *bases, *weights),
        [((fs, height, columns), bf16)],
        specs=[smem, wide, narrow, wide, narrow] + [vmem] * 4,
        scratch=[pltpu.VMEM((RANK, columns), f32)] * 2,
        flops=4 * tokens * depth * RANK,
        room=61,
        grid=(steps,),
    )[0]


def sum_kernel(mixed_ref, out_ref):
    count = out_ref.shape[1]
    total = mixed_ref[0, : 2 * count, :].astype(f32)
    for i in range(1, mixed_ref.shape[0]):
        total = total + mixed_ref[i, : 2 * count, :].astype(f32)
    total = total[:count] + total[count:]
    for j in range(out_ref.shape[0]):
        out_ref[j] = total


def squares_kernel(sums_ref, whole_ref, squares_ref):
    total = sums_ref[0]
    for j in range(1, sums_ref.shape[0]):
        total = total + sums_ref[j]
    whole_ref[...] = total
    squares = jnp.sum(total * total, keepdims=True)
    squares_ref[...] = jnp.broadcast_to(squares[None], squares_ref.shape)


def pack_kernel(whole_ref, first_value, second_value, first_output, second_output, sq_ref, out_ref):
    ranks = first_value.shape[0]
    out_ref[: 2 * ranks, :] = whole_ref[...]
    at = 2 * ranks
    for old_ref in (first_value, second_value, first_output, second_output):
        out_ref[at : at + ranks, :] = old_ref[...]
        at += ranks
    total = sq_ref[0]
    for t in range(1, sq_ref.shape[0]):
        total = total + sq_ref[t]
    out_ref[at:, :] = total


def local(
    saved_hidden,
    grad_value,
    saved_mixed,
    grad_output,
    basis_value,
    basis_output,
    weight_value,
    weight_output,
    first_value,
    second_value,
    first_output,
    second_output,
):
    fs, rep, tp = lax.axis_size("fs"), lax.axis_size("rep"), lax.axis_size("tp")
    fs_index = lax.axis_index("fs").astype(jnp.int32).reshape(1)
    rep_index = lax.axis_index("rep").astype(jnp.int32).reshape(1)
    rows, columns = weight_value.shape
    ranks = first_value.shape[0]

    start = partial(
        rep_index,
        saved_hidden,
        grad_value,
        grad_output,
        saved_mixed,
        (basis_value, basis_output),
        (weight_value, weight_output),
        fs,
        rep,
    )
    mixed = exchange(start, "fs")

    count = 2 * ranks
    summed = call(sum_kernel, (mixed,), [((rep, count, columns), f32)])[0]
    summed = exchange(summed, "rep")
    whole, squares = call(
        squares_kernel, (summed,), [((count, columns), f32), ((tp, 8, columns), f32)]
    )
    squares = exchange(squares, "tp")

    pieces = mixed[:, 2 * count :]
    wholes = exchange(jnp.broadcast_to(pieces[None], (rep, *pieces.shape)), "rep")
    packed = call(
        pack_kernel,
        (whole, first_value, second_value, first_output, second_output, squares),
        [((6 * ranks + 8, columns), f32)],
    )[0]
    gathered = lax.all_gather(packed, "fs")

    block, depth = rows, basis_value.shape[0]
    shapes = [((block, columns), f32)] * 4
    shapes += [((depth, columns), bf16), ((block, depth), bf16)] + [((ranks, columns), f32)] * 4
    return call(
        finish_kernel,
        (fs_index, gathered, wholes, basis_value, basis_output, weight_value, weight_output),
        shapes,
        specs=[smem] + [vmem] * 6,
        scratch=[pltpu.VMEM((RANK, columns), f32)] * 2,
        flops=8 * depth * RANK * columns,
        room=16,
    )


def solution(mesh):
    return jax.shard_map(
        local,
        mesh=mesh,
        in_specs=(
            P(("fs", "rep"), None),
            P(("fs", "rep"), "tp"),
            P(("fs", "rep"), "tp"),
            P(("fs", "rep"), None),
            P(),
            P(),
            P("fs", "tp"),
            P("tp", "fs"),
            P("fs", "tp"),
            P("fs", "tp"),
            P("fs", "tp"),
            P("fs", "tp"),
        ),
        out_specs=(
            P("fs", "tp"),
            P("tp", "fs"),
            P("fs", "tp"),
            P("tp", "fs"),
            P(None, "tp"),
            P("tp", None),
            P("fs", "tp"),
            P("fs", "tp"),
            P("fs", "tp"),
            P("fs", "tp"),
        ),
        check_vma=False,
    )
```

```python
import jax
import jax.numpy as jnp
from jax import lax
from jax.experimental import pallas as pl
from jax.experimental.pallas import tpu as pltpu
from jax.sharding import PartitionSpec as P


AW = 1024
RANK = 128


first_decay = 0.8
second_decay = 0.9
learning_rate = 0.02
norm_epsilon = 1e-06
f32 = jnp.float32
bf16 = jnp.bfloat16
contract_leading = (((0,), (0,)), ((), ()))
contract_trailing = (((1,), (1,)), ((), ()))


def exchange(chunks, axes):
    return lax.all_to_all(chunks, axes, 0, 0, tiled=True)


def split(array):
    upper = array.astype(bf16)
    return upper, (array - upper.astype(f32)).astype(bf16)


def moments(projected, first_old, second_old, clip_factor):
    scaled = clip_factor * projected
    first_new = first_decay * first_old + (1.0 - first_decay) * scaled
    second_new = second_decay * second_old + (1.0 - second_decay) * scaled * scaled
    return (first_new, second_new, first_new / jnp.sqrt(second_new))


def finish_kernel(
    fs_ref,
    rows_ref,
    wholes_ref,
    basis_value_ref,
    basis_output_ref,
    weight_value_ref,
    weight_output_ref,
    step_value_ref,
    step_output_ref,
    new_weight_value_ref,
    new_weight_output_ref,
    copy_value_ref,
    copy_output_ref,
    new_first_value_ref,
    new_second_value_ref,
    new_first_output_ref,
    new_second_output_ref,
    value_ref,
    output_ref,
):
    fs, _, columns = rows_ref.shape
    ranks = new_first_value_ref.shape[0]
    block = weight_value_ref.shape[0]
    cut = wholes_ref.shape[2] // 2
    total = rows_ref[0, 6 * ranks : 6 * ranks + 8, :]
    for i in range(1, fs):
        total = total + rows_ref[i, 6 * ranks : 6 * ranks + 8, :]
    mean_square = jnp.max(total, keepdims=True) / (2 * RANK * AW)
    clip_factor = jnp.minimum(1.0, 1.0 / jnp.sqrt(mean_square + norm_epsilon))

    def part(i, k):
        return rows_ref[i, k * ranks : (k + 1) * ranks, :]

    for i in range(fs):
        here = slice(i * ranks, (i + 1) * ranks)
        value_ref[here, :] = moments(part(i, 0), part(i, 2), part(i, 3), clip_factor)[2]
        output_ref[here, :] = moments(part(i, 1), part(i, 4), part(i, 5), clip_factor)[2]
    own = fs_ref[0]
    first, second, _ = moments(part(own, 0), part(own, 2), part(own, 3), clip_factor)
    new_first_value_ref[...] = first
    new_second_value_ref[...] = second
    first, second, _ = moments(part(own, 1), part(own, 4), part(own, 5), clip_factor)
    new_first_output_ref[...] = first
    new_second_output_ref[...] = second

    value_upper, value_lower = split(value_ref[...])
    output_upper, output_lower = split(output_ref[...].T)

    def value_step(basis):
        return jnp.dot(basis, value_upper, preferred_element_type=f32) + jnp.dot(
            basis, value_lower, preferred_element_type=f32
        )

    def output_step(basis):
        return lax.dot_general(
            output_upper, basis, contract_trailing, preferred_element_type=f32
        ) + lax.dot_general(output_lower, basis, contract_trailing, preferred_element_type=f32)

    own_rows = pl.ds(pl.multiple_of(own * block, block), block)
    step = value_step(basis_value_ref[own_rows, :])
    step_value_ref[...] = step
    new_weight_value_ref[...] = weight_value_ref[...] - learning_rate * step
    step = output_step(basis_output_ref[own_rows, :])
    step_output_ref[...] = step
    new_weight_output_ref[...] = weight_output_ref[...] - learning_rate * step
    for i in range(fs):
        here = slice(i * block, (i + 1) * block)
        whole = wholes_ref[:, i, :cut, :].reshape(block, columns).astype(f32)
        step = value_step(basis_value_ref[here, :])
        copy_value_ref[here, :] = (whole - learning_rate * step).astype(bf16)
        whole = wholes_ref[:, i, cut:, :].reshape(block, columns).astype(f32)
        step = output_step(basis_output_ref[here, :])
        copy_output_ref[:, here] = (whole - learning_rate * step).astype(bf16)


vmem = pl.BlockSpec(memory_space=pltpu.VMEM)
smem = pl.BlockSpec(memory_space=pltpu.SMEM)


def call(kernel, inputs, shapes, specs=None, scratch=(), flops=0, room=8, grid=None):
    outs = tuple(jax.ShapeDtypeStruct(s, t) for s, t in shapes)
    more = {} if grid is None else {"grid": grid}
    return pl.pallas_call(
        kernel,
        out_shape=outs,
        in_specs=[vmem] * len(inputs) if specs is None else specs,
        out_specs=tuple(vmem for _ in outs),
        scratch_shapes=scratch,
        compiler_params=pltpu.CompilerParams(vmem_limit_bytes=room * 2**20),
        cost_estimate=pl.CostEstimate(flops=flops, bytes_accessed=2**20, transcendentals=0),
        **more,
    )(*inputs)


def partial_kernel(
    rep_ref,
    hidden_ref,
    grad_value_ref,
    grad_output_ref,
    mixed_ref,
    basis_value_ref,
    basis_output_ref,
    weight_value_ref,
    weight_output_ref,
    out_ref,
    hidden_sum_ref,
    output_sum_ref,
):
    step = pl.program_id(0)
    for tokens_ref, basis_ref, sum_ref in (
        (hidden_ref, basis_value_ref, hidden_sum_ref),
        (grad_output_ref, basis_output_ref, output_sum_ref),
    ):
        reduced = jnp.dot(tokens_ref[...], basis_ref[...], preferred_element_type=f32)

        @pl.when(step == 0)
        def _():
            sum_ref[...] = reduced

        @pl.when(step > 0)
        def _():
            sum_ref[...] += reduced

    @pl.when(step == pl.num_programs(0) - 1)
    def _():
        products = []
        for sum_ref, other_ref in (
            (hidden_sum_ref, grad_value_ref),
            (output_sum_ref, mixed_ref),
        ):
            upper, lower = split(sum_ref[...])
            other = other_ref[...]
            products.append(
                lax.dot_general(upper, other, contract_leading, preferred_element_type=f32)
                + lax.dot_general(lower, other, contract_leading, preferred_element_type=f32)
            )
        value, output = products
        fs, height, _ = out_ref.shape
        ranks = RANK // fs
        count = 2 * ranks
        cut = (height - 2 * count) // 2
        piece = pl.ds(pl.multiple_of(rep_ref[0] * cut, cut), cut)
        piece_value = weight_value_ref[piece, :].astype(bf16)
        piece_output = weight_output_ref[piece, :].astype(bf16)
        for i in range(fs):
            here = slice(i * ranks, (i + 1) * ranks)
            upper, lower = split(jnp.concatenate([value[here], output[here]]))
            out_ref[i, :count, :] = upper
            out_ref[i, count : 2 * count, :] = lower
            out_ref[i, 2 * count : 2 * count + cut, :] = piece_value
            out_ref[i, 2 * count + cut :, :] = piece_output


def partial(rep_index, hidden, grad_value, grad_output, mixed, bases, weights, fs, rep):
    tokens, depth = hidden.shape
    rows, columns = weights[0].shape
    steps = 4
    block = depth // steps
    wide = pl.BlockSpec((tokens, block), lambda i: (0, i))
    basis = pl.BlockSpec((block, RANK), lambda i: (i, 0))
    narrow = pl.BlockSpec((tokens, columns), lambda i: (0, 0))
    weight = pl.BlockSpec((rows, columns), lambda i: (0, 0))
    height = 4 * (RANK // fs) + 2 * (rows // rep)
    return call(
        partial_kernel,
        (rep_index, hidden, grad_value, grad_output, mixed, *bases, *weights),
        [((fs, height, columns), bf16)],
        specs=[smem, wide, narrow, wide, narrow, basis, basis, weight, weight],
        scratch=[pltpu.VMEM((tokens, RANK), f32)] * 2,
        flops=4 * tokens * depth * RANK,
        room=61,
        grid=(steps,),
    )[0]


def sum_kernel(mixed_ref, out_ref):
    count = out_ref.shape[1]
    total = mixed_ref[0, : 2 * count, :].astype(f32)
    for i in range(1, mixed_ref.shape[0]):
        total = total + mixed_ref[i, : 2 * count, :].astype(f32)
    total = total[:count] + total[count:]
    for j in range(out_ref.shape[0]):
        out_ref[j] = total


def squares_kernel(sums_ref, mixed_ref, whole_ref, squares_ref, spread_ref):
    total = sums_ref[0]
    for j in range(1, sums_ref.shape[0]):
        total = total + sums_ref[j]
    whole_ref[...] = total
    squares = jnp.sum(total * total, keepdims=True)
    squares_ref[...] = jnp.broadcast_to(squares[None], squares_ref.shape)
    rep, _, height, _ = spread_ref.shape
    pieces = mixed_ref[:, mixed_ref.shape[1] - height :, :]
    for j in range(rep):
        spread_ref[j] = pieces


def pack_kernel(whole_ref, first_value, second_value, first_output, second_output, sq_ref, out_ref):
    ranks = first_value.shape[0]
    out_ref[: 2 * ranks, :] = whole_ref[...]
    at = 2 * ranks
    for old_ref in (first_value, second_value, first_output, second_output):
        out_ref[at : at + ranks, :] = old_ref[...]
        at += ranks
    total = sq_ref[0]
    for t in range(1, sq_ref.shape[0]):
        total = total + sq_ref[t]
    out_ref[at:, :] = total


def local(
    saved_hidden,
    grad_value,
    saved_mixed,
    grad_output,
    basis_value,
    basis_output,
    weight_value,
    weight_output,
    first_value,
    second_value,
    first_output,
    second_output,
):
    fs, rep, tp = lax.axis_size("fs"), lax.axis_size("rep"), lax.axis_size("tp")
    fs_index = lax.axis_index("fs").astype(jnp.int32).reshape(1)
    rep_index = lax.axis_index("rep").astype(jnp.int32).reshape(1)
    rows, columns = weight_value.shape
    ranks = first_value.shape[0]

    start = partial(
        rep_index,
        saved_hidden,
        grad_value,
        grad_output,
        saved_mixed,
        (basis_value, basis_output),
        (weight_value, weight_output),
        fs,
        rep,
    )
    mixed = exchange(start, "fs")

    count = 2 * ranks
    summed = call(sum_kernel, (mixed,), [((rep, count, columns), f32)])[0]
    summed = exchange(summed, "rep")
    height = mixed.shape[1] - 2 * count
    whole, squares, spread = call(
        squares_kernel,
        (summed, mixed),
        [
            ((count, columns), f32),
            ((tp, 8, columns), f32),
            ((rep, fs, height, columns), bf16),
        ],
    )
    squares = exchange(squares, "tp")

    wholes = exchange(spread, "rep")
    packed = call(
        pack_kernel,
        (whole, first_value, second_value, first_output, second_output, squares),
        [((6 * ranks + 8, columns), f32)],
    )[0]
    gathered = lax.all_gather(packed, "fs")

    block, depth = rows, basis_value.shape[0]
    shapes = [((block, columns), f32)] * 4
    shapes += [((depth, columns), bf16), ((block, depth), bf16)] + [((ranks, columns), f32)] * 4
    return call(
        finish_kernel,
        (fs_index, gathered, wholes, basis_value, basis_output, weight_value, weight_output),
        shapes,
        specs=[smem] + [vmem] * 6,
        scratch=[pltpu.VMEM((RANK, columns), f32)] * 2,
        flops=8 * depth * RANK * columns,
        room=16,
    )


def solution(mesh):
    return jax.shard_map(
        local,
        mesh=mesh,
        in_specs=(
            P(("fs", "rep"), None),
            P(("fs", "rep"), "tp"),
            P(("fs", "rep"), "tp"),
            P(("fs", "rep"), None),
            P(),
            P(),
            P("fs", "tp"),
            P("tp", "fs"),
            P("fs", "tp"),
            P("fs", "tp"),
            P("fs", "tp"),
            P("fs", "tp"),
        ),
        out_specs=(
            P("fs", "tp"),
            P("tp", "fs"),
            P("fs", "tp"),
            P("tp", "fs"),
            P(None, "tp"),
            P("tp", None),
            P("fs", "tp"),
            P("fs", "tp"),
            P("fs", "tp"),
            P("fs", "tp"),
        ),
        check_vma=False,
    )
```

```python
import jax
import jax.numpy as jnp
from jax import lax
from jax.experimental import pallas as pl
from jax.experimental.pallas import tpu as pltpu
from jax.sharding import PartitionSpec as P


AW = 1024
RANK = 128


first_decay = 0.8
second_decay = 0.9
learning_rate = 0.02
norm_epsilon = 1e-06
f32 = jnp.float32
bf16 = jnp.bfloat16
contract_leading = (((0,), (0,)), ((), ()))
contract_trailing = (((1,), (1,)), ((), ()))


def exchange(chunks, axes):
    return lax.all_to_all(chunks, axes, 0, 0, tiled=True)


def split(array):
    upper = array.astype(bf16)
    return upper, (array - upper.astype(f32)).astype(bf16)


def moments(projected, first_old, second_old, clip_factor):
    scaled = clip_factor * projected
    first_new = first_decay * first_old + (1.0 - first_decay) * scaled
    second_new = second_decay * second_old + (1.0 - second_decay) * scaled * scaled
    return (first_new, second_new, first_new / jnp.sqrt(second_new))


def finish_kernel(
    fs_ref,
    rep_ref,
    rows_ref,
    whole_ref,
    first_value_ref,
    second_value_ref,
    first_output_ref,
    second_output_ref,
    basis_value_ref,
    basis_output_ref,
    weight_value_ref,
    weight_output_ref,
    *refs,
):
    rep = len(refs) - 14
    piece_refs, refs = refs[:rep], refs[rep:]
    (
        step_value_ref,
        step_output_ref,
        new_weight_value_ref,
        new_weight_output_ref,
        copy_value_ref,
        copy_output_ref,
        new_first_value_ref,
        new_second_value_ref,
        new_first_output_ref,
        new_second_output_ref,
        wholes_ref,
        olds_ref,
        value_ref,
        output_ref,
    ) = refs
    fs, height, columns = rows_ref.shape
    ranks = first_value_ref.shape[0]
    count = 2 * ranks
    block = weight_value_ref.shape[0]
    cut = block // rep
    part = 4 * ranks // rep
    run = min(part, ranks)
    for away in range(rep):
        other = lax.rem(rep_ref[0] + away, rep)
        wholes_ref[other] = piece_refs[away][:, : 2 * cut, :]
        old = piece_refs[away][:, 2 * cut :, :].astype(f32)
        olds_ref[other] = old[:, :part] + old[:, part:]

    half = (height - count) // 2
    total = rows_ref[0, count:, :].astype(f32)
    for i in range(1, fs):
        total = total + rows_ref[i, count:, :].astype(f32)
    total = total[:half] + total[half:]
    mean_square = jnp.max(total, keepdims=True) / (2 * RANK * AW)
    clip_factor = jnp.minimum(1.0, 1.0 / jnp.sqrt(mean_square + norm_epsilon))

    def old(i, k):
        runs = [
            olds_ref[at // part, i, at % part : at % part + run, :]
            for at in range(k * ranks, (k + 1) * ranks, run)
        ]
        return jnp.concatenate(runs) if len(runs) > 1 else runs[0]

    for i in range(fs):
        here = slice(i * ranks, (i + 1) * ranks)
        row = rows_ref[i, :count, :].astype(f32)
        value_ref[here, :] = moments(row[:ranks], old(i, 0), old(i, 1), clip_factor)[2]
        output_ref[here, :] = moments(row[ranks:], old(i, 2), old(i, 3), clip_factor)[2]
    first, second, _ = moments(
        whole_ref[:ranks, :], first_value_ref[...], second_value_ref[...], clip_factor
    )
    new_first_value_ref[...] = first
    new_second_value_ref[...] = second
    first, second, _ = moments(
        whole_ref[ranks:, :], first_output_ref[...], second_output_ref[...], clip_factor
    )
    new_first_output_ref[...] = first
    new_second_output_ref[...] = second

    value_upper, value_lower = split(value_ref[...])
    output_upper, output_lower = split(output_ref[...].T)

    def value_step(basis):
        return jnp.dot(basis, value_upper, preferred_element_type=f32) + jnp.dot(
            basis, value_lower, preferred_element_type=f32
        )

    def output_step(basis):
        return lax.dot_general(
            output_upper, basis, contract_trailing, preferred_element_type=f32
        ) + lax.dot_general(output_lower, basis, contract_trailing, preferred_element_type=f32)

    own = fs_ref[0]
    own_rows = pl.ds(pl.multiple_of(own * block, block), block)
    step = value_step(basis_value_ref[own_rows, :])
    step_value_ref[...] = step
    new_weight_value_ref[...] = weight_value_ref[...] - learning_rate * step
    step = output_step(basis_output_ref[own_rows, :])
    step_output_ref[...] = step
    new_weight_output_ref[...] = weight_output_ref[...] - learning_rate * step
    for i in range(fs):
        here = slice(i * block, (i + 1) * block)
        whole = wholes_ref[:, i, :cut, :].reshape(block, columns).astype(f32)
        step = value_step(basis_value_ref[here, :])
        copy_value_ref[here, :] = (whole - learning_rate * step).astype(bf16)
        whole = wholes_ref[:, i, cut:, :].reshape(block, columns).astype(f32)
        step = output_step(basis_output_ref[here, :])
        copy_output_ref[:, here] = (whole - learning_rate * step).astype(bf16)


vmem = pl.BlockSpec(memory_space=pltpu.VMEM)
smem = pl.BlockSpec(memory_space=pltpu.SMEM)


def call(kernel, inputs, shapes, specs=None, scratch=(), flops=0, room=8, grid=None):
    outs = tuple(jax.ShapeDtypeStruct(s, t) for s, t in shapes)
    more = {} if grid is None else {"grid": grid}
    return pl.pallas_call(
        kernel,
        out_shape=outs,
        in_specs=[vmem] * len(inputs) if specs is None else specs,
        out_specs=tuple(vmem for _ in outs),
        scratch_shapes=scratch,
        compiler_params=pltpu.CompilerParams(vmem_limit_bytes=room * 2**20),
        cost_estimate=pl.CostEstimate(flops=flops, bytes_accessed=2**20, transcendentals=0),
        **more,
    )(*inputs)


def partial_kernel(
    rep_ref,
    hidden_ref,
    grad_value_ref,
    grad_output_ref,
    mixed_ref,
    basis_value_ref,
    basis_output_ref,
    weight_value_ref,
    weight_output_ref,
    first_value_ref,
    second_value_ref,
    first_output_ref,
    second_output_ref,
    out_ref,
    hidden_sum_ref,
    output_sum_ref,
    old_ref,
):
    step = pl.program_id(0)
    for tokens_ref, basis_ref, sum_ref in (
        (hidden_ref, basis_value_ref, hidden_sum_ref),
        (grad_output_ref, basis_output_ref, output_sum_ref),
    ):
        reduced = jnp.dot(tokens_ref[...], basis_ref[...], preferred_element_type=f32)

        @pl.when(step == 0)
        def _():
            sum_ref[...] = reduced

        @pl.when(step > 0)
        def _():
            sum_ref[...] += reduced

    @pl.when(step == pl.num_programs(0) - 1)
    def _():
        products = []
        for sum_ref, other_ref in (
            (hidden_sum_ref, grad_value_ref),
            (output_sum_ref, mixed_ref),
        ):
            upper, lower = split(sum_ref[...])
            other = other_ref[...]
            products.append(
                lax.dot_general(upper, other, contract_leading, preferred_element_type=f32)
                + lax.dot_general(lower, other, contract_leading, preferred_element_type=f32)
            )
        value, output = products
        fs = out_ref.shape[0]
        ranks, _ = first_value_ref.shape
        count = 2 * ranks
        rep, part, _ = old_ref.shape
        cut = weight_value_ref.shape[0] // rep
        run = min(part, ranks)
        olds = (first_value_ref, second_value_ref, first_output_ref, second_output_ref)
        for at in range(0, 4 * ranks, run):
            from_row, to_row = at % ranks, at % part
            old_ref[at // part, to_row : to_row + run, :] = olds[at // ranks][
                from_row : from_row + run, :
            ]
        me = rep_ref[0]
        piece = pl.ds(pl.multiple_of(me * cut, cut), cut)
        piece_value = weight_value_ref[piece, :].astype(bf16)
        piece_output = weight_output_ref[piece, :].astype(bf16)
        old = old_ref[me]
        upper = old.astype(bf16).astype(f32)
        piece_old = jnp.concatenate([upper, old - upper]).astype(bf16)
        weights_at = 2 * count
        olds_at = weights_at + 2 * cut
        for i in range(fs):
            here = slice(i * ranks, (i + 1) * ranks)
            upper, lower = split(jnp.concatenate([value[here], output[here]]))
            out_ref[i, :count, :] = upper
            out_ref[i, count:weights_at, :] = lower
            out_ref[i, weights_at : weights_at + cut, :] = piece_value
            out_ref[i, weights_at + cut : olds_at, :] = piece_output
            out_ref[i, olds_at:, :] = piece_old


def partial(rep_index, hidden, grad_value, grad_output, mixed, bases, weights, olds, fs, rep):
    tokens, depth = hidden.shape
    rows, columns = weights[0].shape
    ranks = olds[0].shape[0]
    part = 4 * ranks // rep
    steps = 4
    block = depth // steps
    wide = pl.BlockSpec((tokens, block), lambda i: (0, i))
    basis = pl.BlockSpec((block, RANK), lambda i: (i, 0))
    narrow = pl.BlockSpec((tokens, columns), lambda i: (0, 0))
    weight = pl.BlockSpec((rows, columns), lambda i: (0, 0))
    old = pl.BlockSpec((ranks, columns), lambda i: (0, 0))
    height = 4 * ranks + 2 * (rows // rep) + 2 * part
    return call(
        partial_kernel,
        (rep_index, hidden, grad_value, grad_output, mixed, *bases, *weights, *olds),
        [((fs, height, columns), bf16)],
        specs=[smem, wide, narrow, wide, narrow, basis, basis, weight, weight] + [old] * 4,
        scratch=[pltpu.VMEM((tokens, RANK), f32)] * 2 + [pltpu.VMEM((rep, part, columns), f32)],
        flops=4 * tokens * depth * RANK,
        room=61,
        grid=(steps,),
    )[0]


def sum_kernel(mixed_ref, out_ref, pieces_ref):
    count = out_ref.shape[1]
    total = mixed_ref[0, : 2 * count, :].astype(f32)
    for i in range(1, mixed_ref.shape[0]):
        total = total + mixed_ref[i, : 2 * count, :].astype(f32)
    total = total[:count] + total[count:]
    for j in range(out_ref.shape[0]):
        out_ref[j] = total
    pieces_ref[...] = mixed_ref[:, 2 * count :, :]


def squares_kernel(sums_ref, whole_ref, squares_ref):
    total = sums_ref[0]
    for j in range(1, sums_ref.shape[0]):
        total = total + sums_ref[j]
    whole_ref[...] = total
    squares = jnp.sum(total * total, keepdims=True)
    squares_ref[...] = jnp.broadcast_to(squares[None], squares_ref.shape)


def rows_kernel(whole_ref, squares_ref, out_ref):
    count = whole_ref.shape[0]
    total = squares_ref[0]
    for t in range(1, squares_ref.shape[0]):
        total = total + squares_ref[t]
    total = total[:4]
    upper = total.astype(bf16).astype(f32)
    total = jnp.concatenate([upper, total - upper]).astype(bf16)
    whole = whole_ref[...].astype(bf16)
    for i in range(out_ref.shape[0]):
        out_ref[i, :count, :] = whole
        out_ref[i, count:, :] = total


def local(
    saved_hidden,
    grad_value,
    saved_mixed,
    grad_output,
    basis_value,
    basis_output,
    weight_value,
    weight_output,
    first_value,
    second_value,
    first_output,
    second_output,
):
    fs, rep, tp = lax.axis_size("fs"), lax.axis_size("rep"), lax.axis_size("tp")
    fs_index = lax.axis_index("fs").astype(jnp.int32).reshape(1)
    rep_index = lax.axis_index("rep").astype(jnp.int32).reshape(1)
    rows, columns = weight_value.shape
    ranks = first_value.shape[0]

    olds = (first_value, second_value, first_output, second_output)
    weights = (weight_value, weight_output)
    bases = (basis_value, basis_output)
    start = partial(
        rep_index,
        saved_hidden,
        grad_value,
        grad_output,
        saved_mixed,
        bases,
        weights,
        olds,
        fs,
        rep,
    )
    mixed = exchange(start, "fs")

    count = 2 * ranks
    height = mixed.shape[1] - 2 * count
    summed, piece = call(
        sum_kernel,
        (mixed,),
        [((rep, count, columns), f32), ((fs, height, columns), bf16)],
    )
    summed = exchange(summed, "rep")
    whole, squares = call(
        squares_kernel, (summed,), [((count, columns), f32), ((tp, 8, columns), f32)]
    )
    squares = exchange(squares, "tp")
    rowed = call(rows_kernel, (whole, squares), [((fs, count + 8, columns), bf16)])[0]
    gathered = exchange(rowed, "fs")

    pieces = [piece] + [None] * (rep - 1)
    up = down = piece
    for far in range(1, rep // 2 + 1):
        up = lax.ppermute(up, "rep", [(r, (r + 1) % rep) for r in range(rep)])
        pieces[rep - far] = up
        if 2 * far < rep:
            down = lax.ppermute(down, "rep", [(r, (r - 1) % rep) for r in range(rep)])
            pieces[far] = down

    depth = basis_value.shape[0]
    shapes = [((rows, columns), f32)] * 4
    shapes += [((depth, columns), bf16), ((rows, depth), bf16)] + [((ranks, columns), f32)] * 4
    return call(
        finish_kernel,
        (fs_index, rep_index, gathered, whole, *olds, *bases, *weights, *pieces),
        shapes,
        specs=[smem] * 2 + [vmem] * (10 + rep),
        scratch=[
            pltpu.VMEM((rep, fs, 2 * (rows // rep), columns), bf16),
            pltpu.VMEM((rep, fs, 4 * ranks // rep, columns), f32),
        ]
        + [pltpu.VMEM((RANK, columns), f32)] * 2,
        flops=8 * depth * RANK * columns,
        room=16,
    )


def solution(mesh):
    return jax.shard_map(
        local,
        mesh=mesh,
        in_specs=(
            P(("fs", "rep"), None),
            P(("fs", "rep"), "tp"),
            P(("fs", "rep"), "tp"),
            P(("fs", "rep"), None),
            P(),
            P(),
            P("fs", "tp"),
            P("tp", "fs"),
            P("fs", "tp"),
            P("fs", "tp"),
            P("fs", "tp"),
            P("fs", "tp"),
        ),
        out_specs=(
            P("fs", "tp"),
            P("tp", "fs"),
            P("fs", "tp"),
            P("tp", "fs"),
            P(None, "tp"),
            P("tp", None),
            P("fs", "tp"),
            P("fs", "tp"),
            P("fs", "tp"),
            P("fs", "tp"),
        ),
        check_vma=False,
    )
```

```python
import functools

import jax
import jax.numpy as jnp
from jax import lax
from jax.experimental import pallas as pl
from jax.experimental.pallas import tpu as pltpu
from jax.sharding import PartitionSpec as P


AW = 1024
RANK = 128


first_decay = 0.8
second_decay = 0.9
learning_rate = 0.02
norm_epsilon = 1e-06
f32 = jnp.float32
bf16 = jnp.bfloat16
contract_leading = (((0,), (0,)), ((), ()))
contract_trailing = (((1,), (1,)), ((), ()))


def exchange(chunks, axes):
    return lax.all_to_all(chunks, axes, 0, 0, tiled=True)


def split(array):
    upper = array.astype(bf16)
    return upper, (array - upper.astype(f32)).astype(bf16)


def moments(projected, first_old, second_old, clip_factor):
    scaled = clip_factor * projected
    first_new = first_decay * first_old + (1.0 - first_decay) * scaled
    second_new = second_decay * second_old + (1.0 - second_decay) * scaled * scaled
    return (first_new, second_new, first_new / jnp.sqrt(second_new))


def finish_kernel(
    fs_ref,
    rep_ref,
    rows_ref,
    whole_ref,
    first_value_ref,
    second_value_ref,
    first_output_ref,
    second_output_ref,
    basis_value_ref,
    basis_output_ref,
    weight_value_ref,
    weight_output_ref,
    *refs,
):
    rep = len(refs) - 14
    piece_refs, refs = refs[:rep], refs[rep:]
    (
        step_value_ref,
        step_output_ref,
        new_weight_value_ref,
        new_weight_output_ref,
        copy_value_ref,
        copy_output_ref,
        new_first_value_ref,
        new_second_value_ref,
        new_first_output_ref,
        new_second_output_ref,
        wholes_ref,
        olds_ref,
        value_ref,
        output_ref,
    ) = refs
    fs, height, columns = rows_ref.shape
    ranks = first_value_ref.shape[0]
    count = 2 * ranks
    block = weight_value_ref.shape[0]
    cut = block // rep
    part = 4 * ranks // rep
    run = min(part, ranks)
    for away in range(rep):
        other = lax.rem(rep_ref[0] + away, rep)
        wholes_ref[other] = piece_refs[away][:, : 2 * cut, :]
        old = piece_refs[away][:, 2 * cut :, :].astype(f32)
        olds_ref[other] = old[:, :part] + old[:, part:]

    half = (height - count) // 2
    total = rows_ref[0, count:, :].astype(f32)
    for i in range(1, fs):
        total = total + rows_ref[i, count:, :].astype(f32)
    total = total[:half] + total[half:]
    mean_square = jnp.max(total, keepdims=True) / (2 * RANK * AW)
    clip_factor = jnp.minimum(1.0, 1.0 / jnp.sqrt(mean_square + norm_epsilon))

    def old(i, k):
        runs = [
            olds_ref[at // part, i, at % part : at % part + run, :]
            for at in range(k * ranks, (k + 1) * ranks, run)
        ]
        return jnp.concatenate(runs) if len(runs) > 1 else runs[0]

    for i in range(fs):
        here = slice(i * ranks, (i + 1) * ranks)
        row = rows_ref[i, :count, :].astype(f32)
        value_ref[here, :] = moments(row[:ranks], old(i, 0), old(i, 1), clip_factor)[2]
        output_ref[here, :] = moments(row[ranks:], old(i, 2), old(i, 3), clip_factor)[2]
    first, second, _ = moments(
        whole_ref[:ranks, :], first_value_ref[...], second_value_ref[...], clip_factor
    )
    new_first_value_ref[...] = first
    new_second_value_ref[...] = second
    first, second, _ = moments(
        whole_ref[ranks:, :], first_output_ref[...], second_output_ref[...], clip_factor
    )
    new_first_output_ref[...] = first
    new_second_output_ref[...] = second

    value_upper, value_lower = split(value_ref[...])
    output_upper, output_lower = split(output_ref[...].T)

    def value_step(basis):
        return jnp.dot(basis, value_upper, preferred_element_type=f32) + jnp.dot(
            basis, value_lower, preferred_element_type=f32
        )

    def output_step(basis):
        return lax.dot_general(
            output_upper, basis, contract_trailing, preferred_element_type=f32
        ) + lax.dot_general(output_lower, basis, contract_trailing, preferred_element_type=f32)

    own = fs_ref[0]
    own_rows = pl.ds(pl.multiple_of(own * block, block), block)
    step = value_step(basis_value_ref[own_rows, :])
    step_value_ref[...] = step
    new_weight_value_ref[...] = weight_value_ref[...] - learning_rate * step
    step = output_step(basis_output_ref[own_rows, :])
    step_output_ref[...] = step
    new_weight_output_ref[...] = weight_output_ref[...] - learning_rate * step
    for i in range(fs):
        here = slice(i * block, (i + 1) * block)
        whole = wholes_ref[:, i, :cut, :].reshape(block, columns).astype(f32)
        step = value_step(basis_value_ref[here, :])
        copy_value_ref[here, :] = (whole - learning_rate * step).astype(bf16)
        whole = wholes_ref[:, i, cut:, :].reshape(block, columns).astype(f32)
        step = output_step(basis_output_ref[here, :])
        copy_output_ref[:, here] = (whole - learning_rate * step).astype(bf16)


vmem = pl.BlockSpec(memory_space=pltpu.VMEM)
smem = pl.BlockSpec(memory_space=pltpu.SMEM)


def call(kernel, inputs, shapes, specs=None, scratch=(), flops=0, room=8, grid=None):
    outs = tuple(jax.ShapeDtypeStruct(s, t) for s, t in shapes)
    more = {} if grid is None else {"grid": grid}
    return pl.pallas_call(
        kernel,
        out_shape=outs,
        in_specs=[vmem] * len(inputs) if specs is None else specs,
        out_specs=tuple(vmem for _ in outs),
        scratch_shapes=scratch,
        compiler_params=pltpu.CompilerParams(vmem_limit_bytes=room * 2**20),
        cost_estimate=pl.CostEstimate(flops=flops, bytes_accessed=2**20, transcendentals=0),
        **more,
    )(*inputs)


def partial_kernel(rep_ref, *refs):
    sources, (out_ref, *refs) = refs[:12], refs[12:]
    tokens_refs, held_refs, refs = refs[:2], refs[2:12], refs[12:]
    hidden_sum_ref, output_sum_ref, old_ref, first_sem, token_sem, later_sem = refs
    basis_value_ref, basis_output_ref = held_refs[:2]
    grad_value_ref, mixed_ref, weight_value_ref, weight_output_ref = held_refs[2:6]
    olds = held_refs[6:]
    steps, _, width = tokens_refs[0].shape

    def token_copy(which, k):
        columns = pl.ds(pl.multiple_of(k * width, width), width)
        return pltpu.make_async_copy(
            sources[which].at[:, columns], tokens_refs[which].at[k], token_sem.at[which, k]
        )

    first = [
        pltpu.make_async_copy(sources[2 + n], held_refs[n], first_sem.at[n]) for n in range(2)
    ]
    later = [
        pltpu.make_async_copy(sources[2 + n], held_refs[n], later_sem.at[n - 2])
        for n in range(2, 10)
    ]
    for copy in first:
        copy.start()
    for k in range(steps):
        for which in range(2):
            token_copy(which, k).start()
    for copy in later:
        copy.start()
    hidden_sum_ref[...] = jnp.zeros_like(hidden_sum_ref)
    output_sum_ref[...] = jnp.zeros_like(output_sum_ref)
    for copy in first:
        copy.wait()

    def multiply(k, carry):
        here = pl.ds(pl.multiple_of(k * width, width), width)
        for which, basis_ref, sum_ref in (
            (0, basis_value_ref, hidden_sum_ref),
            (1, basis_output_ref, output_sum_ref),
        ):
            token_copy(which, k).wait()
            sum_ref[...] += jnp.dot(
                tokens_refs[which][k], basis_ref[here, :], preferred_element_type=f32
            )
        return carry

    lax.fori_loop(0, steps, multiply, 0)
    for copy in later:
        copy.wait()
    products = []
    for sum_ref, other_ref in ((hidden_sum_ref, grad_value_ref), (output_sum_ref, mixed_ref)):
        upper, lower = split(sum_ref[...])
        other = other_ref[...]
        products.append(
            lax.dot_general(upper, other, contract_leading, preferred_element_type=f32)
            + lax.dot_general(lower, other, contract_leading, preferred_element_type=f32)
        )
    value, output = products
    fs = out_ref.shape[0]
    ranks = olds[0].shape[0]
    count = 2 * ranks
    rep, part, _ = old_ref.shape
    cut = weight_value_ref.shape[0] // rep
    run = min(part, ranks)
    for at in range(0, 4 * ranks, run):
        from_row, to_row = at % ranks, at % part
        old_ref[at // part, to_row : to_row + run, :] = olds[at // ranks][
            from_row : from_row + run, :
        ]
    me = rep_ref[0]
    piece = pl.ds(pl.multiple_of(me * cut, cut), cut)
    piece_value = weight_value_ref[piece, :].astype(bf16)
    piece_output = weight_output_ref[piece, :].astype(bf16)
    old = old_ref[me]
    upper = old.astype(bf16).astype(f32)
    piece_old = jnp.concatenate([upper, old - upper]).astype(bf16)
    weights_at = 2 * count
    olds_at = weights_at + 2 * cut
    for i in range(fs):
        here = slice(i * ranks, (i + 1) * ranks)
        upper, lower = split(jnp.concatenate([value[here], output[here]]))
        out_ref[i, :count, :] = upper
        out_ref[i, count:weights_at, :] = lower
        out_ref[i, weights_at : weights_at + cut, :] = piece_value
        out_ref[i, weights_at + cut : olds_at, :] = piece_output
        out_ref[i, olds_at:, :] = piece_old


def partial(rep_index, hidden, grad_value, grad_output, mixed, bases, weights, olds, fs, rep):
    tokens, depth = hidden.shape
    rows, columns = weights[0].shape
    ranks = olds[0].shape[0]
    part = 4 * ranks // rep
    steps = depth // 256
    height = 4 * ranks + 2 * (rows // rep) + 2 * part
    held = (*bases, grad_value, mixed, *weights, *olds)
    return call(
        partial_kernel,
        (rep_index, hidden, grad_output, *held),
        [((fs, height, columns), bf16)],
        specs=[smem] + [pl.BlockSpec(memory_space=pl.ANY)] * 12,
        scratch=[pltpu.VMEM((steps, tokens, depth // steps), bf16)] * 2
        + [pltpu.VMEM(a.shape, a.dtype) for a in held]
        + [pltpu.VMEM((tokens, RANK), f32)] * 2
        + [pltpu.VMEM((rep, part, columns), f32)]
        + [pltpu.SemaphoreType.DMA(n) for n in ((2,), (2, steps), (8,))],
        flops=4 * tokens * depth * RANK,
        room=61,
    )[0]


def sum_kernel(mixed_ref, out_ref, pieces_ref):
    count = out_ref.shape[1]
    total = mixed_ref[0, : 2 * count, :].astype(f32)
    for i in range(1, mixed_ref.shape[0]):
        total = total + mixed_ref[i, : 2 * count, :].astype(f32)
    total = (total[:count] + total[count:]).astype(bf16)
    for j in range(out_ref.shape[0]):
        out_ref[j] = total
    pieces_ref[...] = mixed_ref[:, 2 * count :, :]


def rows_kernel(tp, tp_ref, sums_ref, whole_ref, out_ref):
    members, count, columns = sums_ref.shape

    def whole(t):
        total = sums_ref[t].astype(f32)
        for j in range(tp, members, tp):
            total = total + sums_ref[j + t].astype(f32)
        return total

    squares = jnp.zeros((count, columns), f32)
    for t in range(tp):
        total = whole(t)
        squares = squares + total * total
    squares = jnp.broadcast_to(jnp.sum(squares, keepdims=True), (4, columns))
    upper = squares.astype(bf16).astype(f32)
    squares = jnp.concatenate([upper, squares - upper]).astype(bf16)
    own = whole(tp_ref[0])
    whole_ref[...] = own
    own = own.astype(bf16)
    for i in range(out_ref.shape[0]):
        out_ref[i, :count, :] = own
        out_ref[i, count:, :] = squares


def local(
    saved_hidden,
    grad_value,
    saved_mixed,
    grad_output,
    basis_value,
    basis_output,
    weight_value,
    weight_output,
    first_value,
    second_value,
    first_output,
    second_output,
):
    fs, rep, tp = lax.axis_size("fs"), lax.axis_size("rep"), lax.axis_size("tp")
    fs_index = lax.axis_index("fs").astype(jnp.int32).reshape(1)
    rep_index = lax.axis_index("rep").astype(jnp.int32).reshape(1)
    tp_index = lax.axis_index("tp").astype(jnp.int32).reshape(1)
    rows, columns = weight_value.shape
    ranks = first_value.shape[0]

    olds = (first_value, second_value, first_output, second_output)
    weights = (weight_value, weight_output)
    bases = (basis_value, basis_output)
    start = partial(
        rep_index,
        saved_hidden,
        grad_value,
        grad_output,
        saved_mixed,
        bases,
        weights,
        olds,
        fs,
        rep,
    )
    mixed = exchange(start, "fs")

    count = 2 * ranks
    height = mixed.shape[1] - 2 * count
    summed, piece = call(
        sum_kernel,
        (mixed,),
        [((rep * tp, count, columns), bf16), ((fs, height, columns), bf16)],
    )
    summed = exchange(summed, ("rep", "tp"))
    whole, rowed = call(
        functools.partial(rows_kernel, tp),
        (tp_index, summed),
        [((count, columns), f32), ((fs, count + 8, columns), bf16)],
        specs=[smem, vmem],
    )
    gathered = exchange(rowed, "fs")

    pieces = [piece] + [None] * (rep - 1)
    up = down = piece
    for far in range(1, rep // 2 + 1):
        up = lax.ppermute(up, "rep", [(r, (r + 1) % rep) for r in range(rep)])
        pieces[rep - far] = up
        if 2 * far < rep:
            down = lax.ppermute(down, "rep", [(r, (r - 1) % rep) for r in range(rep)])
            pieces[far] = down

    depth = basis_value.shape[0]
    shapes = [((rows, columns), f32)] * 4
    shapes += [((depth, columns), bf16), ((rows, depth), bf16)] + [((ranks, columns), f32)] * 4
    return call(
        finish_kernel,
        (fs_index, rep_index, gathered, whole, *olds, *bases, *weights, *pieces),
        shapes,
        specs=[smem] * 2 + [vmem] * (10 + rep),
        scratch=[
            pltpu.VMEM((rep, fs, 2 * (rows // rep), columns), bf16),
            pltpu.VMEM((rep, fs, 4 * ranks // rep, columns), f32),
        ]
        + [pltpu.VMEM((RANK, columns), f32)] * 2,
        flops=8 * depth * RANK * columns,
        room=16,
    )


def solution(mesh):
    return jax.shard_map(
        local,
        mesh=mesh,
        in_specs=(
            P(("fs", "rep"), None),
            P(("fs", "rep"), "tp"),
            P(("fs", "rep"), "tp"),
            P(("fs", "rep"), None),
            P(),
            P(),
            P("fs", "tp"),
            P("tp", "fs"),
            P("fs", "tp"),
            P("fs", "tp"),
            P("fs", "tp"),
            P("fs", "tp"),
        ),
        out_specs=(
            P("fs", "tp"),
            P("tp", "fs"),
            P("fs", "tp"),
            P("tp", "fs"),
            P(None, "tp"),
            P("tp", None),
            P("fs", "tp"),
            P("fs", "tp"),
            P("fs", "tp"),
            P("fs", "tp"),
        ),
        check_vma=False,
    )
```

```python
import jax
import jax.numpy as jnp
from jax import lax
from jax.experimental import pallas as pl
from jax.experimental.pallas import tpu as pltpu
from jax.sharding import PartitionSpec as P


AW = 1024
RANK = 128


first_decay = 0.8
second_decay = 0.9
learning_rate = 0.02
norm_epsilon = 1e-06
f32 = jnp.float32
bf16 = jnp.bfloat16
contract_leading = (((0,), (0,)), ((), ()))
contract_trailing = (((1,), (1,)), ((), ()))


def exchange(chunks, axes):
    return lax.all_to_all(chunks, axes, 0, 0, tiled=True)


def split(array):
    upper = array.astype(bf16)
    return upper, (array - upper.astype(f32)).astype(bf16)


def moments(projected, first_old, second_old, clip_factor):
    scaled = clip_factor * projected
    first_new = first_decay * first_old + (1.0 - first_decay) * scaled
    second_new = second_decay * second_old + (1.0 - second_decay) * scaled * scaled
    return (first_new, second_new, first_new / jnp.sqrt(second_new))


def finish_kernel(
    fs_ref,
    rep_ref,
    rows_ref,
    squares_ref,
    whole_ref,
    first_value_ref,
    second_value_ref,
    first_output_ref,
    second_output_ref,
    basis_value_ref,
    basis_output_ref,
    weight_value_ref,
    weight_output_ref,
    *refs,
):
    rep = len(refs) - 14
    piece_refs, refs = refs[:rep], refs[rep:]
    (
        step_value_ref,
        step_output_ref,
        new_weight_value_ref,
        new_weight_output_ref,
        copy_value_ref,
        copy_output_ref,
        new_first_value_ref,
        new_second_value_ref,
        new_first_output_ref,
        new_second_output_ref,
        wholes_ref,
        olds_ref,
        value_ref,
        output_ref,
    ) = refs
    fs, _, columns = rows_ref.shape
    ranks = first_value_ref.shape[0]
    count = 2 * ranks
    block = weight_value_ref.shape[0]
    cut = block // rep
    part = 4 * ranks // rep
    run = min(part, ranks)
    for away in range(rep):
        other = lax.rem(rep_ref[0] + away, rep)
        wholes_ref[other] = piece_refs[away][:, : 2 * cut, :]
        old = piece_refs[away][:, 2 * cut :, :].astype(f32)
        olds_ref[other] = old[:, :part] + old[:, part:]

    total = squares_ref[0]
    for t in range(1, squares_ref.shape[0]):
        total = total + squares_ref[t]
    mean_square = jnp.max(total, keepdims=True) / (2 * RANK * AW)
    clip_factor = jnp.minimum(1.0, 1.0 / jnp.sqrt(mean_square + norm_epsilon))

    def old(i, k):
        runs = [
            olds_ref[at // part, i, at % part : at % part + run, :]
            for at in range(k * ranks, (k + 1) * ranks, run)
        ]
        return jnp.concatenate(runs) if len(runs) > 1 else runs[0]

    for i in range(fs):
        here = slice(i * ranks, (i + 1) * ranks)
        row = rows_ref[i, :count, :].astype(f32)
        value_ref[here, :] = moments(row[:ranks], old(i, 0), old(i, 1), clip_factor)[2]
        output_ref[here, :] = moments(row[ranks:], old(i, 2), old(i, 3), clip_factor)[2]
    first, second, _ = moments(
        whole_ref[:ranks, :], first_value_ref[...], second_value_ref[...], clip_factor
    )
    new_first_value_ref[...] = first
    new_second_value_ref[...] = second
    first, second, _ = moments(
        whole_ref[ranks:, :], first_output_ref[...], second_output_ref[...], clip_factor
    )
    new_first_output_ref[...] = first
    new_second_output_ref[...] = second

    value_upper, value_lower = split(value_ref[...])
    output_upper, output_lower = split(output_ref[...].T)

    def value_step(basis):
        return jnp.dot(basis, value_upper, preferred_element_type=f32) + jnp.dot(
            basis, value_lower, preferred_element_type=f32
        )

    def output_step(basis):
        return lax.dot_general(
            output_upper, basis, contract_trailing, preferred_element_type=f32
        ) + lax.dot_general(output_lower, basis, contract_trailing, preferred_element_type=f32)

    own = fs_ref[0]
    own_rows = pl.ds(pl.multiple_of(own * block, block), block)
    step = value_step(basis_value_ref[own_rows, :])
    step_value_ref[...] = step
    new_weight_value_ref[...] = weight_value_ref[...] - learning_rate * step
    step = output_step(basis_output_ref[own_rows, :])
    step_output_ref[...] = step
    new_weight_output_ref[...] = weight_output_ref[...] - learning_rate * step
    for i in range(fs):
        here = slice(i * block, (i + 1) * block)
        whole = wholes_ref[:, i, :cut, :].reshape(block, columns).astype(f32)
        step = value_step(basis_value_ref[here, :])
        copy_value_ref[here, :] = (whole - learning_rate * step).astype(bf16)
        whole = wholes_ref[:, i, cut:, :].reshape(block, columns).astype(f32)
        step = output_step(basis_output_ref[here, :])
        copy_output_ref[:, here] = (whole - learning_rate * step).astype(bf16)


vmem = pl.BlockSpec(memory_space=pltpu.VMEM)
smem = pl.BlockSpec(memory_space=pltpu.SMEM)


def call(kernel, inputs, shapes, specs=None, scratch=(), flops=0, room=8, grid=None):
    outs = tuple(jax.ShapeDtypeStruct(s, t) for s, t in shapes)
    more = {} if grid is None else {"grid": grid}
    return pl.pallas_call(
        kernel,
        out_shape=outs,
        in_specs=[vmem] * len(inputs) if specs is None else specs,
        out_specs=tuple(vmem for _ in outs),
        scratch_shapes=scratch,
        compiler_params=pltpu.CompilerParams(vmem_limit_bytes=room * 2**20),
        cost_estimate=pl.CostEstimate(flops=flops, bytes_accessed=2**20, transcendentals=0),
        **more,
    )(*inputs)


def split_product(reduced, other):
    stacked = jnp.concatenate(split(reduced), axis=1)
    return lax.dot_general(stacked, other, contract_leading, preferred_element_type=f32)


def partial_kernel(
    rep_ref,
    value_ref,
    output_ref,
    weight_value_ref,
    weight_output_ref,
    first_value_ref,
    second_value_ref,
    first_output_ref,
    second_output_ref,
    out_ref,
    old_ref,
):
    fs = out_ref.shape[0]
    ranks = first_value_ref.shape[0]
    count = 2 * ranks
    rep, part, _ = old_ref.shape
    cut = weight_value_ref.shape[0] // rep
    run = min(part, ranks)
    olds = (first_value_ref, second_value_ref, first_output_ref, second_output_ref)
    for at in range(0, 4 * ranks, run):
        from_row, to_row = at % ranks, at % part
        old_ref[at // part, to_row : to_row + run, :] = olds[at // ranks][
            from_row : from_row + run, :
        ]
    me = rep_ref[0]
    piece = pl.ds(pl.multiple_of(me * cut, cut), cut)
    piece_value = weight_value_ref[piece, :].astype(bf16)
    piece_output = weight_output_ref[piece, :].astype(bf16)
    old = old_ref[me]
    upper = old.astype(bf16).astype(f32)
    piece_old = jnp.concatenate([upper, old - upper]).astype(bf16)
    olds_at = count + 2 * cut
    for i in range(fs):
        here = slice(i * ranks, (i + 1) * ranks)
        there = slice(RANK + i * ranks, RANK + (i + 1) * ranks)
        value = value_ref[here, :] + value_ref[there, :]
        output = output_ref[here, :] + output_ref[there, :]
        out_ref[i, :count, :] = jnp.concatenate([value, output]).astype(bf16)
        out_ref[i, count : count + cut, :] = piece_value
        out_ref[i, count + cut : olds_at, :] = piece_output
        out_ref[i, olds_at:, :] = piece_old


def partial(rep_index, hidden, grad_value, grad_output, mixed, bases, weights, olds, fs, rep):
    rows, columns = weights[0].shape
    ranks = olds[0].shape[0]
    part = 4 * ranks // rep
    reduced_hidden = jnp.dot(hidden, bases[0], preferred_element_type=f32)
    reduced_output = jnp.dot(grad_output, bases[1], preferred_element_type=f32)
    value = split_product(reduced_hidden, grad_value)
    output = split_product(reduced_output, mixed)
    height = 2 * ranks + 2 * (rows // rep) + 2 * part
    return call(
        partial_kernel,
        (rep_index, value, output, *weights, *olds),
        [((fs, height, columns), bf16)],
        specs=[smem] + [vmem] * 8,
        scratch=[pltpu.VMEM((rep, part, columns), f32)],
    )[0]


def sum_kernel(mixed_ref, out_ref, pieces_ref):
    count = out_ref.shape[1]
    total = mixed_ref[0, :count, :].astype(f32)
    for i in range(1, mixed_ref.shape[0]):
        total = total + mixed_ref[i, :count, :].astype(f32)
    for j in range(out_ref.shape[0]):
        out_ref[j] = total
    pieces_ref[...] = mixed_ref[:, count:, :]


def rows_kernel(sums_ref, whole_ref, out_ref):
    total = sums_ref[0]
    for j in range(1, sums_ref.shape[0]):
        total = total + sums_ref[j]
    whole_ref[...] = total
    total = total.astype(bf16)
    for i in range(out_ref.shape[0]):
        out_ref[i] = total


def squares_kernel(rows_ref, out_ref):
    total = jnp.zeros(rows_ref.shape[1:], f32)
    for i in range(rows_ref.shape[0]):
        row = rows_ref[i].astype(f32)
        total = total + row * row
    total = jnp.sum(total, keepdims=True)
    out_ref[...] = jnp.broadcast_to(total[None], out_ref.shape)


def local(
    saved_hidden,
    grad_value,
    saved_mixed,
    grad_output,
    basis_value,
    basis_output,
    weight_value,
    weight_output,
    first_value,
    second_value,
    first_output,
    second_output,
):
    fs, rep, tp = lax.axis_size("fs"), lax.axis_size("rep"), lax.axis_size("tp")
    fs_index = lax.axis_index("fs").astype(jnp.int32).reshape(1)
    rep_index = lax.axis_index("rep").astype(jnp.int32).reshape(1)
    rows, columns = weight_value.shape
    ranks = first_value.shape[0]

    olds = (first_value, second_value, first_output, second_output)
    weights = (weight_value, weight_output)
    bases = (basis_value, basis_output)
    start = partial(
        rep_index,
        saved_hidden,
        grad_value,
        grad_output,
        saved_mixed,
        bases,
        weights,
        olds,
        fs,
        rep,
    )
    mixed = exchange(start, "fs")

    count = 2 * ranks
    height = mixed.shape[1] - count
    summed, piece = call(
        sum_kernel,
        (mixed,),
        [((rep, count, columns), f32), ((fs, height, columns), bf16)],
    )
    summed = exchange(summed, "rep")
    whole, rowed = call(
        rows_kernel, (summed,), [((count, columns), f32), ((fs, count, columns), bf16)]
    )

    gathered = exchange(rowed, "fs")
    squares = call(squares_kernel, (gathered,), [((tp, 8, columns), f32)])[0]
    squares = exchange(squares, "tp")

    pieces = [piece] + [None] * (rep - 1)
    up = down = piece
    for far in range(1, rep // 2 + 1):
        up = lax.ppermute(up, "rep", [(r, (r + 1) % rep) for r in range(rep)])
        pieces[rep - far] = up
        if 2 * far < rep:
            down = lax.ppermute(down, "rep", [(r, (r - 1) % rep) for r in range(rep)])
            pieces[far] = down

    depth = basis_value.shape[0]
    shapes = [((rows, columns), f32)] * 4
    shapes += [((depth, columns), bf16), ((rows, depth), bf16)] + [((ranks, columns), f32)] * 4
    return call(
        finish_kernel,
        (fs_index, rep_index, gathered, squares, whole, *olds, *bases, *weights, *pieces),
        shapes,
        specs=[smem] * 2 + [vmem] * (11 + rep),
        scratch=[
            pltpu.VMEM((rep, fs, 2 * (rows // rep), columns), bf16),
            pltpu.VMEM((rep, fs, 4 * ranks // rep, columns), f32),
        ]
        + [pltpu.VMEM((RANK, columns), f32)] * 2,
        flops=8 * depth * RANK * columns,
        room=16,
    )


def solution(mesh):
    return jax.shard_map(
        local,
        mesh=mesh,
        in_specs=(
            P(("fs", "rep"), None),
            P(("fs", "rep"), "tp"),
            P(("fs", "rep"), "tp"),
            P(("fs", "rep"), None),
            P(),
            P(),
            P("fs", "tp"),
            P("tp", "fs"),
            P("fs", "tp"),
            P("fs", "tp"),
            P("fs", "tp"),
            P("fs", "tp"),
        ),
        out_specs=(
            P("fs", "tp"),
            P("tp", "fs"),
            P("fs", "tp"),
            P("tp", "fs"),
            P(None, "tp"),
            P("tp", None),
            P("fs", "tp"),
            P("fs", "tp"),
            P("fs", "tp"),
            P("fs", "tp"),
        ),
        check_vma=False,
    )
```

```python
import jax
import jax.numpy as jnp
from jax import lax
from jax.experimental import pallas as pl
from jax.experimental.pallas import tpu as pltpu
from jax.sharding import PartitionSpec as P


AW = 1024
RANK = 128


first_decay = 0.8
second_decay = 0.9
learning_rate = 0.02
norm_epsilon = 1e-06
f32 = jnp.float32
bf16 = jnp.bfloat16
contract_leading = (((0,), (0,)), ((), ()))
contract_trailing = (((1,), (1,)), ((), ()))


def exchange(chunks, axes):
    return lax.all_to_all(chunks, axes, 0, 0, tiled=True)


def split(array):
    upper = array.astype(bf16)
    return upper, (array - upper.astype(f32)).astype(bf16)


def moments(projected, first_old, second_old, clip_factor):
    scaled = clip_factor * projected
    first_new = first_decay * first_old + (1.0 - first_decay) * scaled
    second_new = second_decay * second_old + (1.0 - second_decay) * scaled * scaled
    return (first_new, second_new, first_new / jnp.sqrt(second_new))


def finish_kernel(
    fs_ref,
    rep_ref,
    rows_ref,
    whole_ref,
    first_value_ref,
    second_value_ref,
    first_output_ref,
    second_output_ref,
    basis_value_ref,
    basis_output_ref,
    weight_value_ref,
    weight_output_ref,
    *refs,
):
    rep = len(refs) - 14
    piece_refs, refs = refs[:rep], refs[rep:]
    (
        step_value_ref,
        step_output_ref,
        new_weight_value_ref,
        new_weight_output_ref,
        copy_value_ref,
        copy_output_ref,
        new_first_value_ref,
        new_second_value_ref,
        new_first_output_ref,
        new_second_output_ref,
        wholes_ref,
        olds_ref,
        value_ref,
        output_ref,
    ) = refs
    fs, height, columns = rows_ref.shape
    ranks = first_value_ref.shape[0]
    count = 2 * ranks
    block = weight_value_ref.shape[0]
    cut = block // rep
    part = 4 * ranks // rep
    run = min(part, ranks)
    for away in range(rep):
        other = lax.rem(rep_ref[0] + away, rep)
        wholes_ref[other] = piece_refs[away][:, : 2 * cut, :]
        old = piece_refs[away][:, 2 * cut :, :].astype(f32)
        olds_ref[other] = old[:, :part] + old[:, part:]

    half = (height - count) // 2
    total = rows_ref[0, count:, :].astype(f32)
    for i in range(1, fs):
        total = total + rows_ref[i, count:, :].astype(f32)
    total = total[:half] + total[half:]
    mean_square = jnp.max(total, keepdims=True) / (2 * RANK * AW)
    clip_factor = jnp.minimum(1.0, 1.0 / jnp.sqrt(mean_square + norm_epsilon))

    def old(i, k):
        runs = [
            olds_ref[at // part, i, at % part : at % part + run, :]
            for at in range(k * ranks, (k + 1) * ranks, run)
        ]
        return jnp.concatenate(runs) if len(runs) > 1 else runs[0]

    for i in range(fs):
        here = slice(i * ranks, (i + 1) * ranks)
        row = rows_ref[i, :count, :].astype(f32)
        value_ref[here, :] = moments(row[:ranks], old(i, 0), old(i, 1), clip_factor)[2]
        output_ref[here, :] = moments(row[ranks:], old(i, 2), old(i, 3), clip_factor)[2]
    first, second, _ = moments(
        whole_ref[:ranks, :], first_value_ref[...], second_value_ref[...], clip_factor
    )
    new_first_value_ref[...] = first
    new_second_value_ref[...] = second
    first, second, _ = moments(
        whole_ref[ranks:, :], first_output_ref[...], second_output_ref[...], clip_factor
    )
    new_first_output_ref[...] = first
    new_second_output_ref[...] = second

    value_upper, value_lower = split(value_ref[...])
    output_upper, output_lower = split(output_ref[...].T)

    def value_step(basis):
        return jnp.dot(basis, value_upper, preferred_element_type=f32) + jnp.dot(
            basis, value_lower, preferred_element_type=f32
        )

    def output_step(basis):
        return lax.dot_general(
            output_upper, basis, contract_trailing, preferred_element_type=f32
        ) + lax.dot_general(output_lower, basis, contract_trailing, preferred_element_type=f32)

    own = fs_ref[0]
    own_rows = pl.ds(pl.multiple_of(own * block, block), block)
    step = value_step(basis_value_ref[own_rows, :])
    step_value_ref[...] = step
    new_weight_value_ref[...] = weight_value_ref[...] - learning_rate * step
    step = output_step(basis_output_ref[own_rows, :])
    step_output_ref[...] = step
    new_weight_output_ref[...] = weight_output_ref[...] - learning_rate * step
    for i in range(fs):
        here = slice(i * block, (i + 1) * block)
        whole = wholes_ref[:, i, :cut, :].reshape(block, columns).astype(f32)
        step = value_step(basis_value_ref[here, :])
        copy_value_ref[here, :] = (whole - learning_rate * step).astype(bf16)
        whole = wholes_ref[:, i, cut:, :].reshape(block, columns).astype(f32)
        step = output_step(basis_output_ref[here, :])
        copy_output_ref[:, here] = (whole - learning_rate * step).astype(bf16)


vmem = pl.BlockSpec(memory_space=pltpu.VMEM)
smem = pl.BlockSpec(memory_space=pltpu.SMEM)


def call(kernel, inputs, shapes, specs=None, scratch=(), flops=0, room=8, grid=None):
    outs = tuple(jax.ShapeDtypeStruct(s, t) for s, t in shapes)
    more = {} if grid is None else {"grid": grid}
    return pl.pallas_call(
        kernel,
        out_shape=outs,
        in_specs=[vmem] * len(inputs) if specs is None else specs,
        out_specs=tuple(vmem for _ in outs),
        scratch_shapes=scratch,
        compiler_params=pltpu.CompilerParams(vmem_limit_bytes=room * 2**20),
        cost_estimate=pl.CostEstimate(flops=flops, bytes_accessed=2**20, transcendentals=0),
        **more,
    )(*inputs)


def split_product(reduced, other):
    stacked = jnp.concatenate(split(reduced), axis=1)
    return lax.dot_general(stacked, other, contract_leading, preferred_element_type=f32)


def partial_kernel(
    rep_ref,
    value_ref,
    output_ref,
    weight_value_ref,
    weight_output_ref,
    first_value_ref,
    second_value_ref,
    first_output_ref,
    second_output_ref,
    out_ref,
    old_ref,
):
    fs = out_ref.shape[0]
    ranks = first_value_ref.shape[0]
    count = 2 * ranks
    rep, part, _ = old_ref.shape
    cut = weight_value_ref.shape[0] // rep
    run = min(part, ranks)
    olds = (first_value_ref, second_value_ref, first_output_ref, second_output_ref)
    for at in range(0, 4 * ranks, run):
        from_row, to_row = at % ranks, at % part
        old_ref[at // part, to_row : to_row + run, :] = olds[at // ranks][
            from_row : from_row + run, :
        ]
    me = rep_ref[0]
    piece = pl.ds(pl.multiple_of(me * cut, cut), cut)
    piece_value = weight_value_ref[piece, :].astype(bf16)
    piece_output = weight_output_ref[piece, :].astype(bf16)
    old = old_ref[me]
    upper = old.astype(bf16).astype(f32)
    piece_old = jnp.concatenate([upper, old - upper]).astype(bf16)
    olds_at = count + 2 * cut
    for i in range(fs):
        here = slice(i * ranks, (i + 1) * ranks)
        there = slice(RANK + i * ranks, RANK + (i + 1) * ranks)
        value = value_ref[here, :] + value_ref[there, :]
        output = output_ref[here, :] + output_ref[there, :]
        out_ref[i, :count, :] = jnp.concatenate([value, output]).astype(bf16)
        out_ref[i, count : count + cut, :] = piece_value
        out_ref[i, count + cut : olds_at, :] = piece_output
        out_ref[i, olds_at:, :] = piece_old


def partial(rep_index, hidden, grad_value, grad_output, mixed, bases, weights, olds, fs, rep):
    rows, columns = weights[0].shape
    ranks = olds[0].shape[0]
    part = 4 * ranks // rep
    reduced_hidden = jnp.dot(hidden, bases[0], preferred_element_type=f32)
    reduced_output = jnp.dot(grad_output, bases[1], preferred_element_type=f32)
    value = split_product(reduced_hidden, grad_value)
    output = split_product(reduced_output, mixed)
    height = 2 * ranks + 2 * (rows // rep) + 2 * part
    return call(
        partial_kernel,
        (rep_index, value, output, *weights, *olds),
        [((fs, height, columns), bf16)],
        specs=[smem] + [vmem] * 8,
        scratch=[pltpu.VMEM((rep, part, columns), f32)],
    )[0]


def sum_kernel(mixed_ref, out_ref, pieces_ref):
    count = out_ref.shape[1]
    total = mixed_ref[0, :count, :].astype(f32)
    for i in range(1, mixed_ref.shape[0]):
        total = total + mixed_ref[i, :count, :].astype(f32)
    for j in range(out_ref.shape[0]):
        out_ref[j] = total
    pieces_ref[...] = mixed_ref[:, count:, :]


def squares_kernel(sums_ref, whole_ref, squares_ref):
    total = sums_ref[0]
    for j in range(1, sums_ref.shape[0]):
        total = total + sums_ref[j]
    whole_ref[...] = total
    squares = jnp.sum(total * total, keepdims=True)
    squares_ref[...] = jnp.broadcast_to(squares[None], squares_ref.shape)


def rows_kernel(whole_ref, squares_ref, out_ref):
    count = whole_ref.shape[0]
    total = squares_ref[0]
    for t in range(1, squares_ref.shape[0]):
        total = total + squares_ref[t]
    total = total[:4]
    upper = total.astype(bf16).astype(f32)
    total = jnp.concatenate([upper, total - upper]).astype(bf16)
    whole = whole_ref[...].astype(bf16)
    for i in range(out_ref.shape[0]):
        out_ref[i, :count, :] = whole
        out_ref[i, count:, :] = total


def local(
    saved_hidden,
    grad_value,
    saved_mixed,
    grad_output,
    basis_value,
    basis_output,
    weight_value,
    weight_output,
    first_value,
    second_value,
    first_output,
    second_output,
):
    fs, rep, tp = lax.axis_size("fs"), lax.axis_size("rep"), lax.axis_size("tp")
    fs_index = lax.axis_index("fs").astype(jnp.int32).reshape(1)
    rep_index = lax.axis_index("rep").astype(jnp.int32).reshape(1)
    rows, columns = weight_value.shape
    ranks = first_value.shape[0]

    olds = (first_value, second_value, first_output, second_output)
    weights = (weight_value, weight_output)
    bases = (basis_value, basis_output)
    start = partial(
        rep_index,
        saved_hidden,
        grad_value,
        grad_output,
        saved_mixed,
        bases,
        weights,
        olds,
        fs,
        rep,
    )
    mixed = exchange(start, "fs")

    count = 2 * ranks
    height = mixed.shape[1] - count
    summed, piece = call(
        sum_kernel,
        (mixed,),
        [((rep, count, columns), f32), ((fs, height, columns), bf16)],
    )
    summed = exchange(summed, "rep")
    whole, squares = call(
        squares_kernel, (summed,), [((count, columns), f32), ((tp, 8, columns), f32)]
    )
    squares = exchange(squares, "tp")
    rowed = call(rows_kernel, (whole, squares), [((fs, count + 8, columns), bf16)])[0]
    gathered = exchange(rowed, "fs")

    pieces = [piece] + [None] * (rep - 1)
    up = down = piece
    for far in range(1, rep // 2 + 1):
        up = lax.ppermute(up, "rep", [(r, (r + 1) % rep) for r in range(rep)])
        pieces[rep - far] = up
        if 2 * far < rep:
            down = lax.ppermute(down, "rep", [(r, (r - 1) % rep) for r in range(rep)])
            pieces[far] = down

    depth = basis_value.shape[0]
    shapes = [((rows, columns), f32)] * 4
    shapes += [((depth, columns), bf16), ((rows, depth), bf16)] + [((ranks, columns), f32)] * 4
    return call(
        finish_kernel,
        (fs_index, rep_index, gathered, whole, *olds, *bases, *weights, *pieces),
        shapes,
        specs=[smem] * 2 + [vmem] * (10 + rep),
        scratch=[
            pltpu.VMEM((rep, fs, 2 * (rows // rep), columns), bf16),
            pltpu.VMEM((rep, fs, 4 * ranks // rep, columns), f32),
        ]
        + [pltpu.VMEM((RANK, columns), f32)] * 2,
        flops=8 * depth * RANK * columns,
        room=16,
    )


def solution(mesh):
    return jax.shard_map(
        local,
        mesh=mesh,
        in_specs=(
            P(("fs", "rep"), None),
            P(("fs", "rep"), "tp"),
            P(("fs", "rep"), "tp"),
            P(("fs", "rep"), None),
            P(),
            P(),
            P("fs", "tp"),
            P("tp", "fs"),
            P("fs", "tp"),
            P("fs", "tp"),
            P("fs", "tp"),
            P("fs", "tp"),
        ),
        out_specs=(
            P("fs", "tp"),
            P("tp", "fs"),
            P("fs", "tp"),
            P("tp", "fs"),
            P(None, "tp"),
            P("tp", None),
            P("fs", "tp"),
            P("fs", "tp"),
            P("fs", "tp"),
            P("fs", "tp"),
        ),
        check_vma=False,
    )
```
